32 devices in a mesh: ep: 8 (over z, core), tp: 4 (over y, x).
Axes of the slice: x: 2, y: 2, z: 4, core: 2. Of those that a mesh axis runs over, the one named last changes fastest.
Arguments:
- query_rows: bfloat16 [6144, 1024], P('ep', 'tp'), may hold values from -600 to 600
- key_rows: bfloat16 [6144, 1024], P('ep', 'tp'), may hold values from -6 to 6
- value_rows: bfloat16 [6144, 1024], P('ep', 'tp'), may hold values from -6 to 6
- cum_gate: float32 [16, 6144], P('tp'), may hold values from -615 to 0, as said below
- out_weight: bfloat16 [1024, 2048], P(None, 'tp'), may hold values from -0.1875 to 0.1875
- moe_input: bfloat16 [1536, 2048], P('ep'), may hold values from -6 to 6
- moe_gain: float32 [2048], replicated, may hold values from 0.1 to 1.9
- routes: int32 [1536, 3], P('ep'), may hold values from 0 to 31, all different within a row; in each aligned block of 192 rows (0 to 191, 192 to 383, ...) at most 36 rows name the same one
- route_weight: float32 [1536, 3], P('ep'), may hold values from 0.2 to 1.5
- expert_gate: bfloat16 [32, 2048, 512], P('ep', None, 'tp'), may hold values from -0.125 to 0.125
- expert_up: bfloat16 [32, 2048, 512], P('ep', None, 'tp'), may hold values from -0.125 to 0.125
- expert_down: bfloat16 [32, 512, 2048], P('ep', None, 'tp'), may hold values from -0.25 to 0.25
- shared_gate: bfloat16 [2048, 512], P(None, 'tp'), may hold values from -0.125 to 0.125
- shared_up: bfloat16 [2048, 512], P(None, 'tp'), may hold values from -0.125 to 0.125
- shared_down: bfloat16 [512, 2048], P(None, 'tp'), may hold values from -0.25 to 0.25
Outputs:
- mixer_out: bfloat16 [6144, 2048], P('ep', 'tp')
- moe_out: bfloat16 [1536, 2048], P('ep', 'tp')
The draws below stay inside these ranges and needn't reach their ends.
Inputs may be any that keep to these rules, and one draw needn't show every extreme that they name: Non-increasing along positions: cum_gate[h, t] is the sum of the log forget gates of head h over positions 0 to t. `routes`: the 3 experts of a token differ. In each aligned block of 192 tokens no expert is named by more than 36 tokens, a bound that some block reaches.
All inputs are finite; a program needn't handle non-finite values.
Results may differ from the reference program's by a relative error of at most 0.0068.
Values may be sent and summed in bfloat16 or wider, within the bound.
A program may use at most 64 MiB of HBM per device.

```python
import math
import jax
import jax.numpy as jnp
import numpy as np
from jax import lax

D = 2048
HEADS = 16
HEAD = 64
FF = 512
FS = 512
EXPERTS = 32
TOP = 3
SEQ_DEV = 768
LENGTH = 6144
MOE_DEV = 192
TOKENS_MOE = 1536
CAP = 36
N_EP = 8


def draw_query_rows(key, part):
    base_key = jax.random.fold_in(key, 7)
    key_normal = jax.random.fold_in(base_key, 0)
    drawn = jnp.clip(jax.random.normal(key_normal, (LENGTH, HEADS * HEAD), jnp.float32), -6.0, 6.0)
    return drawn.astype(jnp.bfloat16)


def draw_cum_gate(key, part):
    base_key = jax.random.fold_in(key, 13)
    key_heads, key_steps, key_blocks = jax.random.split(base_key, 3)
    head_order = jax.random.permutation(key_heads, HEADS)
    fast_count = HEADS // 2
    decay_rates = jnp.where(head_order < fast_count, 1.0 / 40.0, 1.0 / LENGTH).astype(jnp.float32)
    low = jnp.log(0.5)
    high = jnp.log(2.0)
    step_factors = jnp.exp(jax.random.uniform(key_steps, (HEADS, LENGTH), jnp.float32, low, high))
    block_factors = jnp.exp(jax.random.uniform(key_blocks, (HEADS, LENGTH // SEQ_DEV), jnp.float32, low, high))
    block_factors = jnp.repeat(block_factors, SEQ_DEV, axis=1)
    log_gates = -decay_rates[:, None] * step_factors * block_factors
    return jnp.cumsum(log_gates, axis=1).astype(jnp.float32)


def levels(rng, shape, cuts, least, high):
    def one(axis_at, shards_of):
        draws = jax.random.uniform(jax.random.fold_in(jax.random.fold_in(rng, 6), axis_at), (shards_of,), jnp.float32, least / len(cuts), high / len(cuts))
        return jnp.repeat(jnp.exp(draws), shape[axis_at] // shards_of).reshape((-1,) + (1,) * (len(shape) - axis_at - 1))

    loudness = one(*cuts[0])
    for cut in cuts[1:]:
        loudness = loudness * one(*cut)
    return loudness


def deal_out(rng, own, number, rows, amount, top, limit, slope):
    order = jax.random.permutation(rng, amount)
    heavy_load, common = load_shares(amount, rows * top, limit, slope, True), load_shares(amount, rows * top, limit, slope, False)
    places = jnp.arange(amount)

    def named(tallies, turn):
        used = int((tallies > 0).sum())
        fixed = max(1, used // 4)
        shifted = fixed + (places - fixed + turn * (used - fixed)) % max(1, amount - fixed)
        return jnp.zeros((amount,), jnp.int32).at[order[jnp.where(places < fixed, places, shifted)]].set(jnp.asarray(tallies, jnp.int32))

    tallies = jnp.where(number % 4 == 0, named(heavy_load, number // 4), named(common, number - number // 4 - 1))
    mixed = jax.random.permutation(jax.random.fold_in(own, 3), amount)
    donor, receiver = mixed[0:amount // 2 * 2:2], mixed[1:amount // 2 * 2:2]
    margin = jnp.minimum(tallies[donor] - 1, limit - tallies[receiver]) // 2
    margin = jnp.where((donor == order[0]) | (receiver == order[0]) | (tallies[receiver] == 0), 0, jnp.maximum(margin, 0))
    shifted = jax.random.randint(jax.random.fold_in(own, 4), (amount // 2,), 0, 1 << 20) % (margin + 1)
    tallies = tallies.at[donor].add(-shifted).at[receiver].add(shifted)
    members = jnp.searchsorted(jnp.cumsum(tallies), jnp.arange(rows * top), side="right").astype(jnp.int32)
    listing = members.reshape(top, rows).T
    listing = listing[jax.random.permutation(jax.random.fold_in(own, 1), rows)]
    turn = jax.random.randint(jax.random.fold_in(own, 2), (rows, 1), 0, top)
    return jnp.take_along_axis(listing, (jnp.arange(top)[None, :] + turn) % top, axis=1)


def load_shares(amount, total, reach, skew, full):
    portions = [(1 << 20) // math.isqrt(standing ** skew) + 1 for standing in range(1, amount + 1)]
    largest = reach if full else min(reach, max(-(-total // amount), total * portions[0] // sum(portions)))
    least = 1 if total - largest >= amount - 1 else 0
    holding, rest = [largest] + [least] * (amount - 1), total - largest - least * (amount - 1)
    while rest > 0:
        free = [i for i in range(1, amount) if holding[i] < largest] or [i for i in range(1, amount) if holding[i] < reach]
        pool, left = sum([portions[i] for i in free]), rest
        for i in free:
            more = min(reach - holding[i], max(1, left * portions[i] // pool), rest)
            holding[i] = holding[i] + more
            rest = rest - more
    return np.array(holding)


def bell_draw(stream_key, shape, deviation, limit, cuts=(), kind=jnp.bfloat16):
    array = jax.random.normal(stream_key, shape, jnp.float32) * deviation
    if len(cuts) > 0:
        array = levels(stream_key, shape, cuts, -0.22, 0.18) * array
    return jnp.clip(array, min=-limit, max=limit).astype(kind)


def setup_inputs(seed: int = 0) -> dict:
    keys = jax.random.split(jax.random.key(seed), 16)
    query_rows = draw_query_rows(jax.random.fold_in(keys[15], 71), 0)
    key_rows = bell_draw(keys[1], (LENGTH, HEADS * HEAD), 1.0, 6.0, ((0, 8), (1, 4)))
    value_rows = bell_draw(keys[2], (LENGTH, HEADS * HEAD), 1.0, 6.0, ((0, 8), (1, 4)))
    cum_gate = draw_cum_gate(jax.random.fold_in(keys[15], 71), 0)
    out_weight = bell_draw(keys[4], (HEADS * HEAD, D), (HEADS * HEAD) ** -0.5, 0.1875, ((1, 4),))
    moe_input = bell_draw(keys[5], (TOKENS_MOE, D), 1.0, 6.0, ((0, 8),))
    moe_gain = jnp.clip(1.0 + 0.18 * jax.random.normal(keys[6], (D,), jnp.float32), 0.1, 1.9)
    routes_keys = jax.random.split(jax.random.fold_in(keys[7], 1), TOKENS_MOE // MOE_DEV)
    routes_turns = jax.random.permutation(jax.random.fold_in(keys[7], 3), TOKENS_MOE // MOE_DEV)
    routes = jax.vmap(lambda own, number: deal_out(jax.random.fold_in(keys[7], 2), own, number, MOE_DEV, EXPERTS, TOP, CAP, 2))(routes_keys, routes_turns).reshape((TOKENS_MOE, TOP))
    route_weight = jnp.clip(jnp.exp(math.log(1.5) - 2.014903 * jax.random.uniform(keys[8], (TOKENS_MOE, TOP), jnp.float32) ** levels(keys[8], (TOKENS_MOE, TOP), ((0, 8),), -0.2, 0.2)), 0.2, 1.5)
    expert_gate = bell_draw(keys[9], (EXPERTS, D, FF), D ** -0.5, 0.125, ((0, 8), (2, 4)))
    expert_up = bell_draw(keys[10], (EXPERTS, D, FF), D ** -0.5, 0.125, ((0, 8), (2, 4)))
    expert_down = bell_draw(keys[11], (EXPERTS, FF, D), FF ** -0.5, 0.25, ((0, 8), (2, 4)))
    shared_gate = bell_draw(keys[12], (D, FS), D ** -0.5, 0.125, ((1, 4),))
    shared_up = bell_draw(keys[13], (D, FS), D ** -0.5, 0.125, ((1, 4),))
    shared_down = bell_draw(keys[14], (FS, D), FS ** -0.5, 0.25, ((1, 4),))
    return {"query_rows": query_rows, "key_rows": key_rows, "value_rows": value_rows, "cum_gate": cum_gate, "out_weight": out_weight, "moe_input": moe_input, "moe_gain": moe_gain, "routes": routes, "route_weight": route_weight, "expert_gate": expert_gate, "expert_up": expert_up, "expert_down": expert_down, "shared_gate": shared_gate, "shared_up": shared_up, "shared_down": shared_down}


neg_fill = -1e+30
norm_eps = 1e-06

def attention_heads(query_rows, key_rows, value_rows, cum_gate):
    query_span = 128 if LENGTH % 128 == 0 else LENGTH
    query_heads = query_rows.reshape(LENGTH, HEADS, HEAD)
    key_heads = key_rows.reshape(LENGTH, HEADS, HEAD).astype(jnp.float32)
    value_heads = value_rows.reshape(LENGTH, HEADS, HEAD).astype(jnp.float32)
    key_pos = jnp.arange(LENGTH, dtype=jnp.int32)
    scale = HEAD ** (-0.5)

    def one_block(block_index):
        start = (block_index * query_span).astype(jnp.int32)
        query_block = lax.dynamic_slice_in_dim(query_heads, start, query_span, 0).astype(jnp.float32)
        query_gate = lax.dynamic_slice_in_dim(cum_gate, start, query_span, 1)
        scores = jnp.einsum('qhd,khd->hqk', query_block, key_heads) * scale
        scores = scores + query_gate[:, :, None] - cum_gate[:, None, :]
        query_pos = start + jnp.arange(query_span, dtype=jnp.int32)
        causal = key_pos[None, :] <= query_pos[:, None]
        scores = jnp.where(causal[None], scores, neg_fill)
        row_max = lax.optimization_barrier(jnp.max(scores, axis=2, keepdims=True))
        expon = jnp.where(causal[None], jnp.exp(scores - row_max), 0.0)
        denom = lax.optimization_barrier(jnp.sum(expon, axis=2))
        probs = lax.optimization_barrier(expon.astype(jnp.bfloat16)).astype(jnp.float32)
        summed = jnp.einsum('hqk,khd->qhd', probs, value_heads)
        result = summed / jnp.transpose(denom)[:, :, None]
        return result.astype(jnp.bfloat16).reshape(query_span, HEADS * HEAD)
    blocks = lax.map(one_block, jnp.arange(LENGTH // query_span, dtype=jnp.int32))
    return blocks.reshape(LENGTH, HEADS * HEAD)

def experts_branch(moe_input, moe_gain, routes, route_weight, expert_gate, expert_up, expert_down, shared_gate, shared_up, shared_down):
    moe_rows = moe_input.astype(jnp.float32)
    normed = (moe_rows * lax.rsqrt(lax.optimization_barrier(jnp.mean(moe_rows * moe_rows, axis=1, keepdims=True)) + norm_eps) * moe_gain).astype(jnp.bfloat16)
    pair_count = TOKENS_MOE * TOP
    flat_routes = routes.reshape(-1).astype(jnp.int32)
    one_hot = (flat_routes[:, None] == jnp.arange(EXPERTS, dtype=jnp.int32)[None, :]).astype(jnp.int32)
    one_hot = one_hot.reshape(N_EP, MOE_DEV * TOP, EXPERTS)
    ranks = lax.optimization_barrier(jnp.sum(jnp.cumsum(one_hot, axis=1) * one_hot, axis=2)).reshape(-1) - 1
    block_id = jnp.arange(pair_count, dtype=jnp.int32) // (MOE_DEV * TOP)
    slot_index = (flat_routes * (N_EP * CAP) + block_id * CAP + ranks).astype(jnp.int32)
    pair_token = jnp.arange(pair_count, dtype=jnp.int32) // TOP
    slot_token = jnp.full((EXPERTS * N_EP * CAP,), TOKENS_MOE, jnp.int32).at[slot_index].set(pair_token)
    padded = jnp.concatenate([normed, jnp.zeros((1, D), jnp.bfloat16)], axis=0)

    def one_expert(pieces):
        token_index, gate_w, up_w, down_w = pieces
        gathered = padded[token_index]
        gate_val = jnp.dot(gathered, gate_w, preferred_element_type=jnp.float32)
        up_val = jnp.dot(gathered, up_w, preferred_element_type=jnp.float32)
        hidden = (jax.nn.silu(gate_val) * up_val).astype(jnp.bfloat16)
        return jnp.dot(hidden, down_w, preferred_element_type=jnp.float32).astype(jnp.bfloat16)
    results = lax.map(one_expert, (slot_token.reshape(EXPERTS, N_EP * CAP), expert_gate, expert_up, expert_down))
    picked = results.reshape(EXPERTS * N_EP * CAP, D)[slot_index].astype(jnp.float32).reshape(TOKENS_MOE, TOP, D)
    routed = lax.optimization_barrier(jnp.sum(picked * route_weight[:, :, None], axis=1))
    shared_hidden = (jax.nn.silu(jnp.dot(normed, shared_gate, preferred_element_type=jnp.float32)) * jnp.dot(normed, shared_up, preferred_element_type=jnp.float32)).astype(jnp.bfloat16)
    total = routed + jnp.dot(shared_hidden, shared_down, preferred_element_type=jnp.float32)
    return total.astype(jnp.bfloat16)

def reference(query_rows, key_rows, value_rows, cum_gate, out_weight, moe_input, moe_gain, routes, route_weight, expert_gate, expert_up, expert_down, shared_gate, shared_up, shared_down):
    heads_out = attention_heads(query_rows, key_rows, value_rows, cum_gate)
    mixer_out = jnp.dot(heads_out, out_weight, preferred_element_type=jnp.float32).astype(jnp.bfloat16)
    moe_out = experts_branch(moe_input, moe_gain, routes, route_weight, expert_gate, expert_up, expert_down, shared_gate, shared_up, shared_down)
    return (mixer_out, moe_out)
```

```python
import functools

import jax
import jax.numpy as jnp
from jax import lax
from jax.experimental import pallas as pl
from jax.experimental.pallas import tpu as pltpu
from jax.sharding import PartitionSpec as P

HEAD = 64
LANES = 128
CORES = 2

neg_fill = -1e30
norm_eps = 1e-06


def attention_kernel(
    heads,
    q_ref,
    kv_ref,
    gate_ref,
    out_ref,
    held,
    acc,
    row_max,
    up_send,
    side_send,
    recv_sem,
):
    rows = kv_ref.shape[0]
    width = kv_ref.shape[1] // 2
    pairs = width // LANES
    tile = 256 if rows % 256 == 0 else rows
    tiles = rows // tile
    me = lax.axis_index("ep")
    chips = lax.axis_size("ep") // CORES
    chip = me // CORES
    core = me % CORES
    other = 1 - core

    barrier = pltpu.get_barrier_semaphore()

    def greet(index):
        pl.semaphore_signal(barrier, inc=1, device_id={"ep": index})

    greet(chip * CORES + other)

    @pl.when(chip > 0)
    def _():
        greet(me - CORES)

    @pl.when(chip < chips - 1)
    def _():
        greet(me + CORES)

    neighbours = 1 + jnp.where(chip > 0, 1, 0) + jnp.where(chip < chips - 1, 1, 0)
    pl.semaphore_wait(barrier, neighbours)

    def up_copy(src, slot):
        return pltpu.make_async_remote_copy(
            src_ref=src,
            dst_ref=held.at[slot],
            send_sem=up_send.at[slot],
            recv_sem=recv_sem.at[slot],
            device_id={"ep": me + CORES},
        )

    def side_copy(src, slot):
        return pltpu.make_async_remote_copy(
            src_ref=src,
            dst_ref=held.at[slot],
            send_sem=side_send.at[slot],
            recv_sem=recv_sem.at[slot],
            device_id={"ep": chip * CORES + other},
        )

    @pl.when(chip < chips - 1)
    def _():
        up_copy(kv_ref, me).start()

    @pl.when(core == 0)
    def _():
        side_copy(kv_ref, me).start()

    ones = jnp.ones((rows, LANES), jnp.bfloat16)

    def block_step(block, source, first):
        for pair in range(pairs):
            lanes = pl.ds(pair * LANES, LANES)
            value_lanes = pl.ds(width + pair * LANES, LANES)

            def one_tile(index, carry):
                start = pl.multiple_of(index * tile, tile)
                q_rows = pl.ds(start, tile)
                gates = gate_ref[pl.ds(pl.multiple_of(block * rows, rows), rows), lanes]
                keys = jnp.concatenate([source[:, lanes], gates], axis=1)
                values = jnp.concatenate([source[:, value_lanes], ones], axis=1)
                for head in range(2 * pair, min(2 * pair + 2, heads)):
                    scores = lax.dot_general(
                        q_ref[head, q_rows, :],
                        keys,
                        (((1,), (1,)), ((), ())),
                        preferred_element_type=jnp.float32,
                    )
                    if first:
                        q_pos = start + lax.broadcasted_iota(jnp.int32, scores.shape, 0)
                        k_pos = lax.broadcasted_iota(jnp.int32, scores.shape, 1)
                        scores = jnp.where(k_pos <= q_pos, scores, neg_fill)
                        top = jnp.max(scores, axis=1, keepdims=True)
                        new_max = jnp.broadcast_to(top, (tile, LANES))
                    else:
                        old_max = row_max[head, q_rows, :]
                        new_max = jnp.maximum(old_max, jnp.max(scores, axis=1, keepdims=True))
                    probs = jnp.exp(scores - new_max[:, :1]).astype(jnp.bfloat16)
                    add = jnp.dot(probs, values, preferred_element_type=jnp.float32)
                    if not first:
                        keep = jnp.exp(old_max - new_max)
                        add = add + acc[head, q_rows, :] * jnp.concatenate([keep, keep], axis=1)
                    acc[head, q_rows, :] = add
                    row_max[head, q_rows, :] = new_max
                return carry

            lax.fori_loop(0, tiles, one_tile, 0)

    block_step(me, kv_ref, True)

    def remote_step(step, carry):
        turn = step - core + 2
        own_core = turn % 2 == 0
        slot = (chip - turn // 2) * CORES + jnp.where(own_core, core, other)
        landed = held.at[slot]
        side_copy(landed, slot).wait_recv()

        @pl.when(jnp.logical_and(own_core, chip < chips - 1))
        def _():
            up_copy(landed, slot).start()

        @pl.when(own_core)
        def _():
            side_copy(landed, slot).start()

        block_step(slot, landed, False)
        return carry

    lax.fori_loop(0, me, remote_step, 0)

    for head in range(heads):
        pair, part = head // 2, head % 2
        spot = slice(part * HEAD, part * HEAD + HEAD)
        whole = acc[head, :, :LANES] / acc[head, :, LANES:]
        out_ref[:, head * HEAD : (head + 1) * HEAD] = whole[:, spot].astype(out_ref.dtype)

    def finish(step, carry):
        slot = (chip - step) * CORES + core

        @pl.when(chip < chips - 1)
        def _():
            up_copy(held.at[slot], slot).wait_send()

        @pl.when(step > 0)
        def _():
            side_copy(held.at[slot], slot).wait_send()

        return carry

    lax.fori_loop(0, chip + 1, finish, 0)

    @pl.when(core == 0)
    def _():
        side_copy(kv_ref, me).wait_send()


def attention(query_rows, key_rows, value_rows, cum_gate):
    rows, width = query_rows.shape
    heads = width // HEAD
    pairs = (heads + 1) // 2
    ep_count = lax.axis_size("ep")
    padded = pairs * LANES
    if padded > width:
        spare = ((0, 0), (0, padded - width))
        query_rows, key_rows, value_rows = (
            jnp.pad(a, spare) for a in (query_rows, key_rows, value_rows)
        )
    key_value = jnp.concatenate([key_rows, value_rows], axis=1)
    scaled = query_rows * jnp.asarray(HEAD**-0.5, jnp.bfloat16)
    lane = jnp.arange(LANES)
    parts = []
    for head in range(heads):
        pair, part = head // 2, head % 2
        piece = scaled[:, pair * LANES : (pair + 1) * LANES]
        piece = jnp.where((lane // HEAD == part)[None], piece, 0)
        marks = ((lane // 3) == part).astype(jnp.bfloat16)
        parts.append(jnp.concatenate([piece, jnp.broadcast_to(marks, (rows, LANES))], axis=1))
    queries = jnp.stack(parts)
    minus = -cum_gate
    high = lax.reduce_precision(minus, 8, 7)
    rest = minus - high
    mid = lax.reduce_precision(rest, 8, 7)
    low = rest - mid
    terms = jnp.stack([high, mid, low], axis=1).astype(jnp.bfloat16)
    if heads % 2:
        terms = jnp.concatenate([terms, jnp.zeros_like(terms[:1])], axis=0)
    terms = terms.reshape(pairs, 6, cum_gate.shape[1])
    terms = jnp.pad(terms, ((0, 0), (0, LANES - 6), (0, 0)))
    gates = terms.reshape(pairs * LANES, cum_gate.shape[1]).T
    blocks = ep_count * rows * rows * heads
    return pl.pallas_call(
        functools.partial(attention_kernel, heads),
        out_shape=jax.ShapeDtypeStruct((rows, heads * HEAD), jnp.bfloat16),
        in_specs=[pl.BlockSpec(memory_space=pltpu.VMEM)] * 3,
        out_specs=pl.BlockSpec(memory_space=pltpu.VMEM),
        scratch_shapes=[
            pltpu.VMEM((ep_count, rows, 2 * padded), jnp.bfloat16),
            pltpu.VMEM((heads, rows, 2 * LANES), jnp.float32),
            pltpu.VMEM((heads, rows, LANES), jnp.float32),
            pltpu.SemaphoreType.DMA((ep_count,)),
            pltpu.SemaphoreType.DMA((ep_count,)),
            pltpu.SemaphoreType.DMA((ep_count,)),
        ],
        compiler_params=pltpu.CompilerParams(
            collective_id=0, has_side_effects=True, vmem_limit_bytes=48 * 1024 * 1024
        ),
        cost_estimate=pl.CostEstimate(
            flops=blocks * 2 * 512, bytes_accessed=8 * 1024 * 1024, transcendentals=blocks
        ),
        name="attend",
    )(queries, key_value, gates)


def local(
    query_rows,
    key_rows,
    value_rows,
    cum_gate,
    out_weight,
    moe_input,
    moe_gain,
    routes,
    route_weight,
    expert_gate,
    expert_up,
    expert_down,
    shared_gate,
    shared_up,
    shared_down,
):
    heads_out = attention(query_rows, key_rows, value_rows, cum_gate)
    token_count = moe_input.shape[0]
    top_count = routes.shape[1]
    local_experts = expert_gate.shape[0]
    ep_count = lax.axis_size("ep")
    expert_count = local_experts * ep_count
    capacity = 2 * token_count * top_count // expert_count
    column_count = expert_down.shape[2]
    first_column = lax.axis_index("tp") * column_count
    moe_rows = moe_input.astype(jnp.float32)
    normed = (
        moe_rows
        * lax.rsqrt(jnp.mean(moe_rows * moe_rows, axis=1, keepdims=True) + norm_eps)
        * moe_gain
    ).astype(jnp.bfloat16)
    expert_ids = jnp.arange(expert_count, dtype=jnp.int32)
    chosen = routes[:, :, None] == expert_ids[None, None, :]
    named = jnp.any(chosen, axis=1)
    weight_of = jnp.sum(jnp.where(chosen, route_weight[:, :, None], 0.0), axis=1)
    order = jnp.arange(token_count)
    earlier = (order[None, :] < order[:, None]).astype(jnp.bfloat16)
    ranks = jnp.dot(earlier, named.astype(jnp.bfloat16), preferred_element_type=jnp.float32)
    ranks = jnp.where(named, ranks.astype(jnp.int32), -1)
    slots = jnp.arange(capacity, dtype=jnp.int32)
    place = ranks[:, :, None] == slots[None, None, :]
    pick = place.astype(jnp.bfloat16).reshape(token_count, expert_count * capacity)
    own_columns = lax.dynamic_slice_in_dim(normed, first_column, column_count, 1)
    outgoing = lax.dot_general(
        pick, own_columns, (((0,), (0,)), ((), ())), preferred_element_type=jnp.float32
    ).astype(jnp.bfloat16)
    outgoing = outgoing.reshape(ep_count, local_experts, capacity, column_count)
    arrived = lax.all_to_all(outgoing, "ep", split_axis=0, concat_axis=0, tiled=True)
    arrived = lax.all_gather(arrived, "tp", axis=3, tiled=True)
    gate_val = jnp.einsum(
        "aecd,edf->aecf", arrived, expert_gate, preferred_element_type=jnp.float32
    )
    up_val = jnp.einsum("aecd,edf->aecf", arrived, expert_up, preferred_element_type=jnp.float32)
    hidden = (jax.nn.silu(gate_val) * up_val).astype(jnp.bfloat16)
    hidden = lax.all_gather(hidden, "tp", axis=3, tiled=True)
    result = jnp.einsum(
        "aecf,efd->aecd", hidden, expert_down, preferred_element_type=jnp.float32
    ).astype(jnp.bfloat16)
    returned = lax.all_to_all(result, "ep", split_axis=0, concat_axis=0, tiled=True)
    returned = returned.reshape(expert_count * capacity, column_count)
    weight_high = lax.reduce_precision(weight_of, 8, 7)
    weight_low = weight_of - weight_high
    routed = 0.0
    for weight in (weight_high, weight_low):
        spread = jnp.where(place, weight[:, :, None], 0.0).astype(jnp.bfloat16)
        routed = routed + jnp.dot(
            spread.reshape(token_count, expert_count * capacity),
            returned,
            preferred_element_type=jnp.float32,
        )
    shared_hidden = (
        jax.nn.silu(jnp.dot(normed, shared_gate, preferred_element_type=jnp.float32))
        * jnp.dot(normed, shared_up, preferred_element_type=jnp.float32)
    ).astype(jnp.bfloat16)
    heads_all, shared_all = (
        lax.all_gather(heads_out, "tp", axis=1, tiled=True),
        lax.all_gather(shared_hidden, "tp", axis=1, tiled=True),
    )
    mixer_sum = jnp.dot(heads_all, out_weight, preferred_element_type=jnp.float32)
    moe_total = routed + jnp.dot(shared_all, shared_down, preferred_element_type=jnp.float32)
    return (mixer_sum.astype(jnp.bfloat16), moe_total.astype(jnp.bfloat16))


def solution(mesh):
    placed = (
        P("ep", "tp"),
        P("ep", "tp"),
        P("ep", "tp"),
        P("tp", None),
        P(None, "tp"),
        P("ep", None),
        P(),
        P("ep", None),
        P("ep", None),
        P("ep", None, "tp"),
        P("ep", None, "tp"),
        P("ep", None, "tp"),
        P(None, "tp"),
        P(None, "tp"),
        P(None, "tp"),
    )
    return jax.shard_map(
        local, mesh=mesh, in_specs=placed, out_specs=(P("ep", "tp"), P("ep", "tp")), check_vma=False
    )
```

```python
import functools

import jax
import jax.numpy as jnp
from jax import lax
from jax.experimental import pallas as pl
from jax.experimental.pallas import tpu as pltpu
from jax.sharding import PartitionSpec as P

HEAD = 64
LANES = 128
CORES = 2

neg_fill = -1e30
norm_eps = 1e-06


def attention_kernel(
    heads,
    q_ref,
    kv_ref,
    gate_ref,
    normed_ref,
    out_ref,
    tokens,
    held,
    acc,
    row_max,
    up_send,
    side_send,
    recv_sem,
    chip_send,
    plane_send,
    piece_recv,
    block_send,
    block_recv,
    own_sem,
):
    rows = kv_ref.shape[0]
    width = kv_ref.shape[1] // 2
    pairs = width // LANES
    tile = 256 if rows % 256 == 0 else rows
    tiles = rows // tile
    me = lax.axis_index("ep")
    chips = lax.axis_size("ep") // CORES
    chip = me // CORES
    core = me % CORES
    other = 1 - core

    barrier = pltpu.get_barrier_semaphore()

    def loop(count, body):
        def step(index, carry):
            body(index)
            return carry

        lax.fori_loop(0, count, step, 0)

    def greet(**where):
        pl.semaphore_signal(barrier, inc=1, device_id=where)

    tp_count = lax.axis_size("tp")
    tp_me = lax.axis_index("tp")
    columns = normed_ref.shape[1] // tp_count

    def chip_at(turn):
        return lax.rem(chip + turn + 1, chips)

    def tp_at(turn):
        return lax.rem(tp_me + turn + 1, tp_count)

    greet(ep=chip * CORES + other)
    loop(chips - 1, lambda turn: greet(ep=chip_at(turn) * CORES + core))
    loop(tp_count - 1, lambda turn: greet(tp=tp_at(turn)))
    pl.semaphore_wait(barrier, chips + tp_count - 1)

    def up_copy(src, slot):
        return pltpu.make_async_remote_copy(
            src_ref=src,
            dst_ref=held.at[slot],
            send_sem=up_send.at[slot],
            recv_sem=recv_sem.at[slot],
            device_id={"ep": me + CORES},
        )

    def far_copy(target):
        return pltpu.make_async_remote_copy(
            src_ref=kv_ref,
            dst_ref=held.at[me],
            send_sem=up_send.at[target * CORES + core],
            recv_sem=recv_sem.at[me],
            device_id={"ep": target * CORES + core},
        )

    def side_copy(src, slot):
        return pltpu.make_async_remote_copy(
            src_ref=src,
            dst_ref=held.at[slot],
            send_sem=side_send.at[slot],
            recv_sem=recv_sem.at[slot],
            device_id={"ep": chip * CORES + other},
        )

    def lanes_of(index):
        return pl.ds(pl.multiple_of(index * columns, columns), columns)

    def chip_copy(target):
        return pltpu.make_async_remote_copy(
            src_ref=normed_ref.at[:, lanes_of(tp_me)],
            dst_ref=tokens.at[me, :, lanes_of(tp_me)],
            send_sem=chip_send.at[target],
            recv_sem=piece_recv.at[me, tp_me],
            device_id={"ep": target * CORES + core},
        )

    def plane_copy(slot, piece, target):
        place = tokens.at[slot, :, lanes_of(piece)]
        return pltpu.make_async_remote_copy(
            src_ref=place,
            dst_ref=place,
            send_sem=plane_send.at[slot, target],
            recv_sem=piece_recv.at[slot, piece],
            device_id={"tp": target},
        )

    def block_copy(src, slot):
        return pltpu.make_async_remote_copy(
            src_ref=src,
            dst_ref=tokens.at[slot],
            send_sem=block_send.at[slot],
            recv_sem=block_recv.at[slot],
            device_id={"ep": chip * CORES + other},
        )

    loop(chips - 1, lambda turn: chip_copy(chip_at(turn)).start())

    @pl.when(chip < chips - 1)
    def _():
        up_copy(kv_ref, me).start()

    reach = chips // 2
    far_count = jnp.maximum(chips - 1 - reach - chip, 0)
    loop(far_count, lambda turn: far_copy(chips - 1 - turn).start())

    @pl.when(core == 0)
    def _():
        side_copy(kv_ref, me).start()

    block_copy(normed_ref, me).start()
    own_copy = pltpu.make_async_copy(normed_ref, tokens.at[me], own_sem)
    own_copy.start()

    def spread_pieces(turn):
        slot = chip_at(turn) * CORES + core
        plane_copy(slot, tp_me, tp_me).wait_recv()
        loop(tp_count - 1, lambda way: plane_copy(slot, tp_me, tp_at(way)).start())

    def share_blocks(turn):
        slot = chip_at(turn) * CORES + core
        loop(tp_count - 1, lambda way: plane_copy(slot, tp_at(way), tp_me).wait_recv())
        block_copy(tokens.at[slot], slot).start()

    ones = jnp.ones((rows, LANES), jnp.bfloat16)

    def block_step(block, source, first):
        for pair in range(pairs):
            lanes = pl.ds(pair * LANES, LANES)
            value_lanes = pl.ds(width + pair * LANES, LANES)

            def one_tile(index, carry):
                start = pl.multiple_of(index * tile, tile)
                q_rows = pl.ds(start, tile)
                gates = gate_ref[pl.ds(pl.multiple_of(block * rows, rows), rows), lanes]
                keys = jnp.concatenate([source[:, lanes], gates], axis=1)
                values = jnp.concatenate([source[:, value_lanes], ones], axis=1)
                for head in range(2 * pair, min(2 * pair + 2, heads)):
                    scores = lax.dot_general(
                        q_ref[head, q_rows, :],
                        keys,
                        (((1,), (1,)), ((), ())),
                        preferred_element_type=jnp.float32,
                    )
                    if first:
                        q_pos = start + lax.broadcasted_iota(jnp.int32, scores.shape, 0)
                        k_pos = lax.broadcasted_iota(jnp.int32, scores.shape, 1)
                        scores = jnp.where(k_pos <= q_pos, scores, neg_fill)
                        top = jnp.max(scores, axis=1, keepdims=True)
                        new_max = jnp.broadcast_to(top, (tile, LANES))
                    else:
                        old_max = row_max[head, q_rows, :]
                        new_max = jnp.maximum(old_max, jnp.max(scores, axis=1, keepdims=True))
                    probs = jnp.exp(scores - new_max[:, :1]).astype(jnp.bfloat16)
                    add = jnp.dot(probs, values, preferred_element_type=jnp.float32)
                    if not first:
                        keep = jnp.exp(old_max - new_max)
                        add = add + acc[head, q_rows, :] * jnp.concatenate([keep, keep], axis=1)
                    acc[head, q_rows, :] = add
                    row_max[head, q_rows, :] = new_max
                return carry

            lax.fori_loop(0, tiles, one_tile, 0)

    block_step(me, kv_ref, True)
    loop(chips - 1, spread_pieces)

    @pl.when(me == 0)
    def _():
        loop(chips - 1, share_blocks)

    def remote_step(step, carry):
        turn = step - core + 2
        own_core = turn % 2 == 0
        order = turn // 2
        back = jnp.where(order < 2, order, chip + 2 - order)
        slot = (chip - back) * CORES + jnp.where(own_core, core, other)
        landed = held.at[slot]
        side_copy(landed, slot).wait_recv()

        @pl.when(jnp.logical_and(own_core, jnp.logical_and(chip < chips - 1, back < reach)))
        def _():
            up_copy(landed, slot).start()

        @pl.when(own_core)
        def _():
            side_copy(landed, slot).start()

        @pl.when(step == jnp.maximum(me - 2, 0))
        def _():
            loop(chips - 1, share_blocks)

        block_step(slot, landed, False)
        return carry

    lax.fori_loop(0, me, remote_step, 0)

    for head in range(heads):
        pair, part = head // 2, head % 2
        spot = slice(part * HEAD, part * HEAD + HEAD)
        whole = acc[head, :, :LANES] / acc[head, :, LANES:]
        out_ref[:, head * HEAD : (head + 1) * HEAD] = whole[:, spot].astype(out_ref.dtype)

    def finish(step):
        slot = (chip - step) * CORES + core

        @pl.when(jnp.logical_and(chip < chips - 1, step < reach))
        def _():
            up_copy(held.at[slot], slot).wait_send()

        @pl.when(step > 0)
        def _():
            side_copy(held.at[slot], slot).wait_send()

    loop(chip + 1, finish)
    loop(far_count, lambda turn: far_copy(chips - 1 - turn).wait_send())

    @pl.when(core == 0)
    def _():
        side_copy(kv_ref, me).wait_send()

    def finish_tokens(turn):
        target = chip_at(turn)
        slot = target * CORES + core
        chip_copy(target).wait_send()
        loop(tp_count - 1, lambda way: plane_copy(slot, tp_me, tp_at(way)).wait_send())
        block_copy(tokens.at[slot], slot).wait_send()

    loop(chips - 1, finish_tokens)
    block_copy(normed_ref, me).wait_send()

    def finish_blocks(index):
        slot = index * CORES + other
        block_copy(tokens.at[slot], slot).wait_recv()

    loop(chips, finish_blocks)
    own_copy.wait()


def exchange_kernel(count, *refs):
    sources, targets = refs[:count], refs[count : 2 * count]
    send_sem, recv_sem, own_sem = refs[2 * count :]
    tp_count = lax.axis_size("tp")
    tp_me = lax.axis_index("tp")
    barrier = pltpu.get_barrier_semaphore()
    ways = [lax.rem(tp_me + turn, tp_count) for turn in range(1, tp_count)]
    for way in ways:
        pl.semaphore_signal(barrier, inc=1, device_id={"tp": way})
    pl.semaphore_wait(barrier, tp_count - 1)

    def copy(index, way, owner):
        return pltpu.make_async_remote_copy(
            src_ref=sources[index],
            dst_ref=targets[index].at[owner],
            send_sem=send_sem.at[index, way],
            recv_sem=recv_sem.at[index, owner],
            device_id={"tp": way},
        )

    for index in range(count):
        for way in ways:
            copy(index, way, tp_me).start()
    own = [
        pltpu.make_async_copy(sources[index], targets[index].at[tp_me], own_sem.at[index])
        for index in range(count)
    ]
    for one in own:
        one.start()
    for one in own:
        one.wait()
    for index in range(count):
        for way in ways:
            copy(index, way, way).wait_recv()
            copy(index, way, tp_me).wait_send()


def exchange(*arrays):
    tp_count = lax.axis_size("tp")
    count = len(arrays)
    return pl.pallas_call(
        functools.partial(exchange_kernel, count),
        out_shape=[jax.ShapeDtypeStruct((tp_count,) + a.shape, a.dtype) for a in arrays],
        in_specs=[pl.BlockSpec(memory_space=pltpu.VMEM)] * count,
        out_specs=[pl.BlockSpec(memory_space=pltpu.VMEM)] * count,
        scratch_shapes=[
            pltpu.SemaphoreType.DMA((count, tp_count)),
            pltpu.SemaphoreType.DMA((count, tp_count)),
            pltpu.SemaphoreType.DMA((count,)),
        ],
        compiler_params=pltpu.CompilerParams(collective_id=1, has_side_effects=True),
        cost_estimate=pl.CostEstimate(flops=0, bytes_accessed=24 * 1024 * 1024, transcendentals=0),
        name="exchange",
    )(*arrays)


def attention(query_rows, key_rows, value_rows, cum_gate, normed):
    rows, width = query_rows.shape
    heads = width // HEAD
    pairs = (heads + 1) // 2
    ep_count = lax.axis_size("ep")
    padded = pairs * LANES
    if padded > width:
        spare = ((0, 0), (0, padded - width))
        query_rows, key_rows, value_rows = (
            jnp.pad(a, spare) for a in (query_rows, key_rows, value_rows)
        )
    key_value = jnp.concatenate([key_rows, value_rows], axis=1)
    scaled = query_rows * jnp.asarray(HEAD**-0.5, jnp.bfloat16)
    lane = jnp.arange(LANES)
    parts = []
    for head in range(heads):
        pair, part = head // 2, head % 2
        piece = scaled[:, pair * LANES : (pair + 1) * LANES]
        piece = jnp.where((lane // HEAD == part)[None], piece, 0)
        marks = ((lane // 3) == part).astype(jnp.bfloat16)
        parts.append(jnp.concatenate([piece, jnp.broadcast_to(marks, (rows, LANES))], axis=1))
    queries = jnp.stack(parts)
    minus = -cum_gate
    high = lax.reduce_precision(minus, 8, 7)
    rest = minus - high
    mid = lax.reduce_precision(rest, 8, 7)
    low = rest - mid
    terms = jnp.stack([high, mid, low], axis=1).astype(jnp.bfloat16)
    if heads % 2:
        terms = jnp.concatenate([terms, jnp.zeros_like(terms[:1])], axis=0)
    terms = terms.reshape(pairs, 6, cum_gate.shape[1])
    terms = jnp.pad(terms, ((0, 0), (0, LANES - 6), (0, 0)))
    gates = terms.reshape(pairs * LANES, cum_gate.shape[1]).T
    blocks = ep_count * rows * rows * heads
    return pl.pallas_call(
        functools.partial(attention_kernel, heads),
        out_shape=[
            jax.ShapeDtypeStruct((rows, heads * HEAD), jnp.bfloat16),
            jax.ShapeDtypeStruct((ep_count,) + normed.shape, jnp.bfloat16),
        ],
        in_specs=[pl.BlockSpec(memory_space=pltpu.VMEM)] * 4,
        out_specs=[
            pl.BlockSpec(memory_space=pltpu.VMEM),
            pl.BlockSpec(memory_space=pl.ANY),
        ],
        scratch_shapes=[
            pltpu.VMEM((ep_count, rows, 2 * padded), jnp.bfloat16),
            pltpu.VMEM((heads, rows, 2 * LANES), jnp.float32),
            pltpu.VMEM((heads, rows, LANES), jnp.float32),
            pltpu.SemaphoreType.DMA((ep_count,)),
            pltpu.SemaphoreType.DMA((ep_count,)),
            pltpu.SemaphoreType.DMA((ep_count,)),
            pltpu.SemaphoreType.DMA((ep_count,)),
            pltpu.SemaphoreType.DMA((ep_count, lax.axis_size("tp"))),
            pltpu.SemaphoreType.DMA((ep_count, lax.axis_size("tp"))),
            pltpu.SemaphoreType.DMA((ep_count,)),
            pltpu.SemaphoreType.DMA((ep_count,)),
            pltpu.SemaphoreType.DMA,
        ],
        compiler_params=pltpu.CompilerParams(
            collective_id=0, has_side_effects=True, vmem_limit_bytes=48 * 1024 * 1024
        ),
        cost_estimate=pl.CostEstimate(
            flops=blocks * 2 * 512, bytes_accessed=8 * 1024 * 1024, transcendentals=blocks
        ),
        name="attend",
    )(queries, key_value, gates, normed)


def local(
    query_rows,
    key_rows,
    value_rows,
    cum_gate,
    out_weight,
    moe_input,
    moe_gain,
    routes,
    route_weight,
    expert_gate,
    expert_up,
    expert_down,
    shared_gate,
    shared_up,
    shared_down,
):
    token_count = moe_input.shape[0]
    top_count = routes.shape[1]
    local_experts = expert_gate.shape[0]
    ep_count = lax.axis_size("ep")
    expert_count = local_experts * ep_count
    capacity = 2 * token_count * top_count // expert_count
    column_count = expert_down.shape[2]
    first_column = lax.axis_index("tp") * column_count
    moe_rows = moe_input.astype(jnp.float32)
    normed = (
        moe_rows
        * lax.rsqrt(jnp.mean(moe_rows * moe_rows, axis=1, keepdims=True) + norm_eps)
        * moe_gain
    ).astype(jnp.bfloat16)
    expert_ids = jnp.arange(expert_count, dtype=jnp.int32)
    chosen = routes[:, :, None] == expert_ids[None, None, :]
    named = jnp.any(chosen, axis=1)
    weight_of = jnp.sum(jnp.where(chosen, route_weight[:, :, None], 0.0), axis=1)
    order = jnp.arange(token_count)
    earlier = (order[None, :] < order[:, None]).astype(jnp.bfloat16)
    ranks = jnp.dot(earlier, named.astype(jnp.bfloat16), preferred_element_type=jnp.float32)
    ranks = jnp.where(named, ranks.astype(jnp.int32), -1)
    slots = jnp.arange(capacity, dtype=jnp.int32)
    place = ranks[:, :, None] == slots[None, None, :]
    heads_out, tokens = attention(query_rows, key_rows, value_rows, cum_gate, normed)
    all_ranks = lax.all_gather(
        ranks.astype(jnp.bfloat16).reshape(token_count, ep_count, local_experts), "ep", axis=0
    )
    mine = lax.dynamic_index_in_dim(all_ranks, lax.axis_index("ep"), 2, keepdims=False)
    pick = mine.transpose(0, 2, 1)[:, :, None, :] == slots.astype(jnp.bfloat16)[None, None, :, None]
    pick = pick.astype(jnp.bfloat16).reshape(ep_count, local_experts * capacity, token_count)
    arrived = jnp.einsum("ast,atd->asd", pick, tokens, preferred_element_type=jnp.float32)
    arrived = arrived.astype(jnp.bfloat16).reshape(ep_count, local_experts, capacity, -1)
    gate_val = jnp.einsum(
        "aecd,edf->aecf", arrived, expert_gate, preferred_element_type=jnp.float32
    )
    up_val = jnp.einsum("aecd,edf->aecf", arrived, expert_up, preferred_element_type=jnp.float32)
    hidden = (jax.nn.silu(gate_val) * up_val).astype(jnp.bfloat16)
    shared_hidden = (
        jax.nn.silu(jnp.dot(normed, shared_gate, preferred_element_type=jnp.float32))
        * jnp.dot(normed, shared_up, preferred_element_type=jnp.float32)
    ).astype(jnp.bfloat16)
    slot_count = ep_count * local_experts * capacity
    by_expert = hidden.transpose(1, 0, 2, 3).reshape(slot_count, hidden.shape[3])
    hidden, shared_all = exchange(by_expert, shared_hidden)
    hidden = hidden.transpose(1, 0, 2).reshape(local_experts, ep_count * capacity, -1)
    shared_all = shared_all.transpose(1, 0, 2).reshape(token_count, -1)
    result = jnp.einsum("esf,efd->esd", hidden, expert_down, preferred_element_type=jnp.float32)
    result = result.astype(jnp.bfloat16).reshape(local_experts, ep_count, capacity, column_count)
    result = result.transpose(1, 0, 2, 3)
    returned = lax.all_to_all(result, "ep", split_axis=0, concat_axis=0, tiled=True)
    returned = returned.reshape(expert_count * capacity, column_count)
    weight_high = lax.reduce_precision(weight_of, 8, 7)
    weight_low = weight_of - weight_high
    routed = 0.0
    for weight in (weight_high, weight_low):
        spread = jnp.where(place, weight[:, :, None], 0.0).astype(jnp.bfloat16)
        routed = routed + jnp.dot(
            spread.reshape(token_count, expert_count * capacity),
            returned,
            preferred_element_type=jnp.float32,
        )
    heads_all = lax.all_gather(heads_out, "tp", axis=1, tiled=True)
    mixer_sum = jnp.dot(heads_all, out_weight, preferred_element_type=jnp.float32)
    moe_total = routed + jnp.dot(shared_all, shared_down, preferred_element_type=jnp.float32)
    return (mixer_sum.astype(jnp.bfloat16), moe_total.astype(jnp.bfloat16))


def solution(mesh):
    placed = (
        P("ep", "tp"),
        P("ep", "tp"),
        P("ep", "tp"),
        P("tp", None),
        P(None, "tp"),
        P("ep", None),
        P(),
        P("ep", None),
        P("ep", None),
        P("ep", None, "tp"),
        P("ep", None, "tp"),
        P("ep", None, "tp"),
        P(None, "tp"),
        P(None, "tp"),
        P(None, "tp"),
    )
    return jax.shard_map(
        local, mesh=mesh, in_specs=placed, out_specs=(P("ep", "tp"), P("ep", "tp")), check_vma=False
    )
```

```python
import functools

import jax
import jax.numpy as jnp
from jax import lax
from jax.experimental import pallas as pl
from jax.experimental.pallas import tpu as pltpu
from jax.sharding import PartitionSpec as P

HEAD = 64
LANES = 128
CORES = 2

neg_fill = -1e30
norm_eps = 1e-06


def attention_kernel(
    heads,
    q_ref,
    kv_ref,
    gate_ref,
    normed_ref,
    rank_ref,
    out_ref,
    tokens,
    picks,
    held,
    acc,
    row_max,
    up_send,
    side_send,
    recv_sem,
    chip_send,
    plane_send,
    piece_recv,
    block_send,
    block_recv,
    own_sem,
    rank_send,
    rank_recv,
):
    rows = kv_ref.shape[0]
    width = kv_ref.shape[1] // 2
    pairs = width // LANES
    tile = 256 if rows % 256 == 0 else rows
    tiles = rows // tile
    me = lax.axis_index("ep")
    chips = lax.axis_size("ep") // CORES
    chip = me // CORES
    core = me % CORES
    other = 1 - core

    barrier = pltpu.get_barrier_semaphore()

    def loop(count, body):
        def step(index, carry):
            body(index)
            return carry

        lax.fori_loop(0, count, step, 0)

    def greet(**where):
        pl.semaphore_signal(barrier, inc=1, device_id=where)

    tp_count = lax.axis_size("tp")
    tp_me = lax.axis_index("tp")
    columns = normed_ref.shape[1] // tp_count

    def chip_at(turn):
        return lax.rem(chip + turn + 1, chips)

    def tp_at(turn):
        return lax.rem(tp_me + turn + 1, tp_count)

    ep_count = chips * CORES

    def ep_at(turn):
        return lax.rem(me + turn + 1, ep_count)

    loop(ep_count - 1, lambda turn: greet(ep=ep_at(turn)))
    loop(tp_count - 1, lambda turn: greet(tp=tp_at(turn)))
    pl.semaphore_wait(barrier, ep_count + tp_count - 2)

    def rank_copy(target, owner):
        return pltpu.make_async_remote_copy(
            src_ref=rank_ref.at[target],
            dst_ref=picks.at[owner],
            send_sem=rank_send.at[target],
            recv_sem=rank_recv.at[owner],
            device_id={"ep": target},
        )

    def up_copy(src, slot):
        return pltpu.make_async_remote_copy(
            src_ref=src,
            dst_ref=held.at[slot],
            send_sem=up_send.at[slot],
            recv_sem=recv_sem.at[slot],
            device_id={"ep": me + CORES},
        )

    def far_copy(target):
        return pltpu.make_async_remote_copy(
            src_ref=kv_ref,
            dst_ref=held.at[me],
            send_sem=up_send.at[target * CORES + core],
            recv_sem=recv_sem.at[me],
            device_id={"ep": target * CORES + core},
        )

    def side_copy(src, slot):
        return pltpu.make_async_remote_copy(
            src_ref=src,
            dst_ref=held.at[slot],
            send_sem=side_send.at[slot],
            recv_sem=recv_sem.at[slot],
            device_id={"ep": chip * CORES + other},
        )

    def lanes_of(index):
        return pl.ds(pl.multiple_of(index * columns, columns), columns)

    def chip_copy(target):
        return pltpu.make_async_remote_copy(
            src_ref=normed_ref.at[:, lanes_of(tp_me)],
            dst_ref=tokens.at[me, :, lanes_of(tp_me)],
            send_sem=chip_send.at[target],
            recv_sem=piece_recv.at[me, tp_me],
            device_id={"ep": target * CORES + core},
        )

    def plane_copy(slot, piece, target):
        place = tokens.at[slot, :, lanes_of(piece)]
        return pltpu.make_async_remote_copy(
            src_ref=place,
            dst_ref=place,
            send_sem=plane_send.at[slot, target],
            recv_sem=piece_recv.at[slot, piece],
            device_id={"tp": target},
        )

    def block_copy(src, slot):
        return pltpu.make_async_remote_copy(
            src_ref=src,
            dst_ref=tokens.at[slot],
            send_sem=block_send.at[slot],
            recv_sem=block_recv.at[slot],
            device_id={"ep": chip * CORES + other},
        )

    loop(chips - 1, lambda turn: chip_copy(chip_at(turn)).start())

    @pl.when(chip < chips - 1)
    def _():
        up_copy(kv_ref, me).start()

    reach = chips // 2
    far_count = jnp.maximum(chips - 1 - reach - chip, 0)
    loop(far_count, lambda turn: far_copy(chips - 1 - turn).start())

    @pl.when(core == 0)
    def _():
        side_copy(kv_ref, me).start()

    block_copy(normed_ref, me).start()
    own_copy = pltpu.make_async_copy(normed_ref, tokens.at[me], own_sem)
    own_copy.start()
    loop(ep_count - 1, lambda turn: rank_copy(ep_at(turn), me).start())
    picks[me] = rank_ref[me]

    def spread_pieces(turn):
        slot = chip_at(turn) * CORES + core
        plane_copy(slot, tp_me, tp_me).wait_recv()
        loop(tp_count - 1, lambda way: plane_copy(slot, tp_me, tp_at(way)).start())

    def share_blocks(turn):
        slot = chip_at(turn) * CORES + core
        loop(tp_count - 1, lambda way: plane_copy(slot, tp_at(way), tp_me).wait_recv())
        block_copy(tokens.at[slot], slot).start()

    ones = jnp.ones((rows, LANES), jnp.bfloat16)

    def block_step(block, source, first):
        for pair in range(pairs):
            lanes = pl.ds(pair * LANES, LANES)
            value_lanes = pl.ds(width + pair * LANES, LANES)

            def one_tile(index, carry):
                start = pl.multiple_of(index * tile, tile)
                q_rows = pl.ds(start, tile)
                gates = gate_ref[pl.ds(pl.multiple_of(block * rows, rows), rows), lanes]
                keys = jnp.concatenate([source[:, lanes], gates], axis=1)
                values = jnp.concatenate([source[:, value_lanes], ones], axis=1)
                for head in range(2 * pair, min(2 * pair + 2, heads)):
                    scores = lax.dot_general(
                        q_ref[head, q_rows, :],
                        keys,
                        (((1,), (1,)), ((), ())),
                        preferred_element_type=jnp.float32,
                    )
                    if first:
                        q_pos = start + lax.broadcasted_iota(jnp.int32, scores.shape, 0)
                        k_pos = lax.broadcasted_iota(jnp.int32, scores.shape, 1)
                        scores = jnp.where(k_pos <= q_pos, scores, neg_fill)
                        top = jnp.max(scores, axis=1, keepdims=True)
                        new_max = jnp.broadcast_to(top, (tile, LANES))
                    else:
                        old_max = row_max[head, q_rows, :]
                        new_max = jnp.maximum(old_max, jnp.max(scores, axis=1, keepdims=True))
                    probs = jnp.exp(scores - new_max[:, :1]).astype(jnp.bfloat16)
                    add = jnp.dot(probs, values, preferred_element_type=jnp.float32)
                    if not first:
                        keep = jnp.exp(old_max - new_max)
                        add = add + acc[head, q_rows, :] * jnp.concatenate([keep, keep], axis=1)
                    acc[head, q_rows, :] = add
                    row_max[head, q_rows, :] = new_max
                return carry

            lax.fori_loop(0, tiles, one_tile, 0)

    block_step(me, kv_ref, True)
    loop(chips - 1, spread_pieces)

    @pl.when(me == 0)
    def _():
        loop(chips - 1, share_blocks)

    def remote_step(step, carry):
        turn = step - core + 2
        own_core = turn % 2 == 0
        order = turn // 2
        back = jnp.where(order < 2, order, chip + 2 - order)
        slot = (chip - back) * CORES + jnp.where(own_core, core, other)
        landed = held.at[slot]
        side_copy(landed, slot).wait_recv()

        @pl.when(jnp.logical_and(own_core, jnp.logical_and(chip < chips - 1, back < reach)))
        def _():
            up_copy(landed, slot).start()

        @pl.when(own_core)
        def _():
            side_copy(landed, slot).start()

        @pl.when(step == jnp.maximum(me - 2, 0))
        def _():
            loop(chips - 1, share_blocks)

        block_step(slot, landed, False)
        return carry

    lax.fori_loop(0, me, remote_step, 0)

    for head in range(heads):
        pair, part = head // 2, head % 2
        spot = slice(part * HEAD, part * HEAD + HEAD)
        whole = acc[head, :, :LANES] / acc[head, :, LANES:]
        out_ref[:, head * HEAD : (head + 1) * HEAD] = whole[:, spot].astype(out_ref.dtype)

    def finish(step):
        slot = (chip - step) * CORES + core

        @pl.when(jnp.logical_and(chip < chips - 1, step < reach))
        def _():
            up_copy(held.at[slot], slot).wait_send()

        @pl.when(step > 0)
        def _():
            side_copy(held.at[slot], slot).wait_send()

    loop(chip + 1, finish)
    loop(far_count, lambda turn: far_copy(chips - 1 - turn).wait_send())

    @pl.when(core == 0)
    def _():
        side_copy(kv_ref, me).wait_send()

    def finish_tokens(turn):
        target = chip_at(turn)
        slot = target * CORES + core
        chip_copy(target).wait_send()
        loop(tp_count - 1, lambda way: plane_copy(slot, tp_me, tp_at(way)).wait_send())
        block_copy(tokens.at[slot], slot).wait_send()

    loop(chips - 1, finish_tokens)
    block_copy(normed_ref, me).wait_send()

    def finish_blocks(index):
        slot = index * CORES + other
        block_copy(tokens.at[slot], slot).wait_recv()

    loop(chips, finish_blocks)
    own_copy.wait()

    def finish_ranks(turn):
        rank_copy(ep_at(turn), me).wait_send()
        rank_copy(ep_at(turn), ep_at(turn)).wait_recv()

    loop(ep_count - 1, finish_ranks)


def exchange_kernel(count, *refs):
    sources, targets = refs[:count], refs[count : 2 * count]
    send_sem, recv_sem, own_sem = refs[2 * count :]
    tp_count = lax.axis_size("tp")
    tp_me = lax.axis_index("tp")
    barrier = pltpu.get_barrier_semaphore()
    ways = [lax.rem(tp_me + turn, tp_count) for turn in range(1, tp_count)]
    for way in ways:
        pl.semaphore_signal(barrier, inc=1, device_id={"tp": way})
    pl.semaphore_wait(barrier, tp_count - 1)

    def place(index, owner):
        span = sources[index].shape[1]
        if span % LANES:
            return targets[index].at[owner]
        return targets[index].at[:, pl.ds(pl.multiple_of(owner * span, span), span)]

    def copy(index, way, owner):
        return pltpu.make_async_remote_copy(
            src_ref=sources[index],
            dst_ref=place(index, owner),
            send_sem=send_sem.at[index, way],
            recv_sem=recv_sem.at[index, owner],
            device_id={"tp": way},
        )

    for index in range(count):
        for way in ways:
            copy(index, way, tp_me).start()
    own = [
        pltpu.make_async_copy(sources[index], place(index, tp_me), own_sem.at[index])
        for index in range(count)
    ]
    for one in own:
        one.start()
    for one in own:
        one.wait()
    for index in range(count):
        for way in ways:
            copy(index, way, way).wait_recv()
            copy(index, way, tp_me).wait_send()


def exchange(collective_id, *arrays):
    tp_count = lax.axis_size("tp")
    count = len(arrays)

    def gathered(a):
        rows, span = a.shape
        shape = (tp_count, rows, span) if span % LANES else (rows, tp_count * span)
        return jax.ShapeDtypeStruct(shape, a.dtype)

    results = pl.pallas_call(
        functools.partial(exchange_kernel, count),
        out_shape=[gathered(a) for a in arrays],
        in_specs=[pl.BlockSpec(memory_space=pltpu.VMEM)] * count,
        out_specs=[pl.BlockSpec(memory_space=pltpu.VMEM)] * count,
        scratch_shapes=[
            pltpu.SemaphoreType.DMA((count, tp_count)),
            pltpu.SemaphoreType.DMA((count, tp_count)),
            pltpu.SemaphoreType.DMA((count,)),
        ],
        compiler_params=pltpu.CompilerParams(collective_id=collective_id, has_side_effects=True),
        cost_estimate=pl.CostEstimate(flops=0, bytes_accessed=24 * 1024 * 1024, transcendentals=0),
        name="exchange",
    )(*arrays)
    return [
        r if r.ndim == 2 else r.transpose(1, 0, 2).reshape(r.shape[1], -1) for r in results
    ]


def attention(query_rows, key_rows, value_rows, cum_gate, normed, ranks):
    rows, width = query_rows.shape
    heads = width // HEAD
    pairs = (heads + 1) // 2
    ep_count = lax.axis_size("ep")
    padded = pairs * LANES
    if padded > width:
        spare = ((0, 0), (0, padded - width))
        query_rows, key_rows, value_rows = (
            jnp.pad(a, spare) for a in (query_rows, key_rows, value_rows)
        )
    key_value = jnp.concatenate([key_rows, value_rows], axis=1)
    scaled = query_rows * jnp.asarray(HEAD**-0.5, jnp.bfloat16)
    lane = jnp.arange(LANES)
    parts = []
    for head in range(heads):
        pair, part = head // 2, head % 2
        piece = scaled[:, pair * LANES : (pair + 1) * LANES]
        piece = jnp.where((lane // HEAD == part)[None], piece, 0)
        marks = ((lane // 3) == part).astype(jnp.bfloat16)
        parts.append(jnp.concatenate([piece, jnp.broadcast_to(marks, (rows, LANES))], axis=1))
    queries = jnp.stack(parts)
    minus = -cum_gate
    high = lax.reduce_precision(minus, 8, 7)
    rest = minus - high
    mid = lax.reduce_precision(rest, 8, 7)
    low = rest - mid
    terms = jnp.concatenate([high, mid, low], axis=0).astype(jnp.bfloat16)
    source = jnp.arange(3 * heads)
    spot = (source % heads // 2) * LANES + (source % heads % 2) * 3 + source // heads
    layout = (spot[:, None] == jnp.arange(padded)[None, :]).astype(jnp.bfloat16)
    gates = lax.dot_general(
        terms, layout, (((0,), (0,)), ((), ())), preferred_element_type=jnp.float32
    ).astype(jnp.bfloat16)
    blocks = ep_count * rows * rows * heads
    return pl.pallas_call(
        functools.partial(attention_kernel, heads),
        out_shape=[
            jax.ShapeDtypeStruct((rows, heads * HEAD), jnp.bfloat16),
            jax.ShapeDtypeStruct((ep_count,) + normed.shape, jnp.bfloat16),
            jax.ShapeDtypeStruct(ranks.shape, jnp.bfloat16),
        ],
        in_specs=[pl.BlockSpec(memory_space=pltpu.VMEM)] * 5,
        out_specs=[
            pl.BlockSpec(memory_space=pltpu.VMEM),
            pl.BlockSpec(memory_space=pl.ANY),
            pl.BlockSpec(memory_space=pltpu.VMEM),
        ],
        scratch_shapes=[
            pltpu.VMEM((ep_count, rows, 2 * padded), jnp.bfloat16),
            pltpu.VMEM((heads, rows, 2 * LANES), jnp.float32),
            pltpu.VMEM((heads, rows, LANES), jnp.float32),
            pltpu.SemaphoreType.DMA((ep_count,)),
            pltpu.SemaphoreType.DMA((ep_count,)),
            pltpu.SemaphoreType.DMA((ep_count,)),
            pltpu.SemaphoreType.DMA((ep_count,)),
            pltpu.SemaphoreType.DMA((ep_count, lax.axis_size("tp"))),
            pltpu.SemaphoreType.DMA((ep_count, lax.axis_size("tp"))),
            pltpu.SemaphoreType.DMA((ep_count,)),
            pltpu.SemaphoreType.DMA((ep_count,)),
            pltpu.SemaphoreType.DMA,
            pltpu.SemaphoreType.DMA((ep_count,)),
            pltpu.SemaphoreType.DMA((ep_count,)),
        ],
        compiler_params=pltpu.CompilerParams(
            collective_id=0, has_side_effects=True, vmem_limit_bytes=48 * 1024 * 1024
        ),
        cost_estimate=pl.CostEstimate(
            flops=blocks * 2 * 512, bytes_accessed=8 * 1024 * 1024, transcendentals=blocks
        ),
        name="attend",
    )(queries, key_value, gates, normed, ranks)


def local(
    query_rows,
    key_rows,
    value_rows,
    cum_gate,
    out_weight,
    moe_input,
    moe_gain,
    routes,
    route_weight,
    expert_gate,
    expert_up,
    expert_down,
    shared_gate,
    shared_up,
    shared_down,
):
    token_count = moe_input.shape[0]
    top_count = routes.shape[1]
    local_experts = expert_gate.shape[0]
    ep_count = lax.axis_size("ep")
    expert_count = local_experts * ep_count
    capacity = 2 * token_count * top_count // expert_count
    column_count = expert_down.shape[2]
    first_column = lax.axis_index("tp") * column_count
    moe_rows = moe_input.astype(jnp.float32)
    normed = (
        moe_rows
        * lax.rsqrt(jnp.mean(moe_rows * moe_rows, axis=1, keepdims=True) + norm_eps)
        * moe_gain
    ).astype(jnp.bfloat16)
    expert_ids = jnp.arange(expert_count, dtype=jnp.int32)
    chosen = routes[:, :, None] == expert_ids[None, None, :]
    named = jnp.any(chosen, axis=1)
    weight_of = jnp.sum(jnp.where(chosen, route_weight[:, :, None], 0.0), axis=1)
    order = jnp.arange(token_count)
    earlier = (order[None, :] < order[:, None]).astype(jnp.bfloat16)
    ranks = jnp.dot(earlier, named.astype(jnp.bfloat16), preferred_element_type=jnp.float32)
    ranks = jnp.where(named, ranks.astype(jnp.int32), -1)
    slots = jnp.arange(capacity, dtype=jnp.int32)
    place = ranks[:, :, None] == slots[None, None, :]
    rank_rows = ranks.astype(jnp.bfloat16).T.reshape(ep_count, local_experts, token_count)
    heads_out, tokens, mine = attention(
        query_rows, key_rows, value_rows, cum_gate, normed, rank_rows
    )
    pick = mine[:, :, None, :] == slots.astype(jnp.bfloat16)[None, None, :, None]
    pick = pick.astype(jnp.bfloat16).reshape(ep_count, local_experts * capacity, token_count)
    arrived = jnp.einsum("ast,atd->asd", pick, tokens, preferred_element_type=jnp.float32)
    arrived = arrived.astype(jnp.bfloat16).reshape(ep_count, local_experts, capacity, -1)
    gate_val = jnp.einsum(
        "aecd,edf->aecf", arrived, expert_gate, preferred_element_type=jnp.float32
    )
    up_val = jnp.einsum("aecd,edf->aecf", arrived, expert_up, preferred_element_type=jnp.float32)
    hidden = (jax.nn.silu(gate_val) * up_val).astype(jnp.bfloat16)
    shared_hidden = (
        jax.nn.silu(jnp.dot(normed, shared_gate, preferred_element_type=jnp.float32))
        * jnp.dot(normed, shared_up, preferred_element_type=jnp.float32)
    ).astype(jnp.bfloat16)
    slot_count = ep_count * local_experts * capacity
    by_expert = hidden.transpose(1, 0, 2, 3).reshape(slot_count, hidden.shape[3])
    hidden, shared_all = exchange(1, by_expert, shared_hidden)
    hidden = hidden.reshape(local_experts, ep_count * capacity, -1)
    result = jnp.einsum("esf,efd->esd", hidden, expert_down, preferred_element_type=jnp.float32)
    result = result.astype(jnp.bfloat16).reshape(local_experts, ep_count, capacity, column_count)
    result = result.transpose(1, 0, 2, 3)
    result, heads_out = lax.optimization_barrier((result, heads_out))
    returned = lax.all_to_all(result, "ep", split_axis=0, concat_axis=0, tiled=True)
    returned = returned.reshape(expert_count * capacity, column_count)
    weight_high = lax.reduce_precision(weight_of, 8, 7)
    weight_low = weight_of - weight_high
    routed = 0.0
    for weight in (weight_high, weight_low):
        spread = jnp.where(place, weight[:, :, None], 0.0).astype(jnp.bfloat16)
        routed = routed + jnp.dot(
            spread.reshape(token_count, expert_count * capacity),
            returned,
            preferred_element_type=jnp.float32,
        )
    (heads_all,) = exchange(2, heads_out)
    mixer_sum = jnp.dot(heads_all, out_weight, preferred_element_type=jnp.float32)
    moe_total = routed + jnp.dot(shared_all, shared_down, preferred_element_type=jnp.float32)
    return (mixer_sum.astype(jnp.bfloat16), moe_total.astype(jnp.bfloat16))


def solution(mesh):
    placed = (
        P("ep", "tp"),
        P("ep", "tp"),
        P("ep", "tp"),
        P("tp", None),
        P(None, "tp"),
        P("ep", None),
        P(),
        P("ep", None),
        P("ep", None),
        P("ep", None, "tp"),
        P("ep", None, "tp"),
        P("ep", None, "tp"),
        P(None, "tp"),
        P(None, "tp"),
        P(None, "tp"),
    )
    return jax.shard_map(
        local, mesh=mesh, in_specs=placed, out_specs=(P("ep", "tp"), P("ep", "tp")), check_vma=False
    )
```

```python
import functools

import jax
import jax.numpy as jnp
from jax import lax
from jax.experimental import pallas as pl
from jax.experimental.pallas import tpu as pltpu
from jax.sharding import PartitionSpec as P

HEAD = 64
LANES = 128
CORES = 2

neg_fill = -1e30
norm_eps = 1e-06


def attention_kernel(
    heads,
    q_ref,
    kv_ref,
    gate_ref,
    normed_ref,
    rank_ref,
    out_ref,
    tokens,
    picks,
    held,
    acc,
    row_max,
    up_send,
    side_send,
    recv_sem,
    chip_send,
    plane_send,
    piece_recv,
    block_send,
    block_recv,
    own_sem,
    rank_send,
    rank_recv,
):
    rows = kv_ref.shape[0]
    width = kv_ref.shape[1] // 2
    pairs = width // LANES
    tile = 256 if rows % 256 == 0 else rows
    tiles = rows // tile
    me = lax.axis_index("ep")
    chips = lax.axis_size("ep") // CORES
    chip = me // CORES
    core = me % CORES
    other = 1 - core

    barrier = pltpu.get_barrier_semaphore()

    def loop(count, body):
        def step(index, carry):
            body(index)
            return carry

        lax.fori_loop(0, count, step, 0)

    def greet(**where):
        pl.semaphore_signal(barrier, inc=1, device_id=where)

    tp_count = lax.axis_size("tp")
    tp_me = lax.axis_index("tp")
    columns = normed_ref.shape[1] // tp_count

    def chip_at(turn):
        return lax.rem(chip + turn + 1, chips)

    def tp_at(turn):
        return lax.rem(tp_me + turn + 1, tp_count)

    ep_count = chips * CORES

    def ep_at(turn):
        return lax.rem(me + turn + 1, ep_count)

    loop(ep_count - 1, lambda turn: greet(ep=ep_at(turn)))
    loop(tp_count - 1, lambda turn: greet(tp=tp_at(turn)))
    pl.semaphore_wait(barrier, ep_count + tp_count - 2)

    def rank_copy(target, owner):
        return pltpu.make_async_remote_copy(
            src_ref=rank_ref.at[target],
            dst_ref=picks.at[owner],
            send_sem=rank_send.at[target],
            recv_sem=rank_recv.at[owner],
            device_id={"ep": target},
        )

    def up_copy(src, slot):
        return pltpu.make_async_remote_copy(
            src_ref=src,
            dst_ref=held.at[slot],
            send_sem=up_send.at[slot],
            recv_sem=recv_sem.at[slot],
            device_id={"ep": me + CORES},
        )

    def side_copy(src, slot):
        return pltpu.make_async_remote_copy(
            src_ref=src,
            dst_ref=held.at[slot],
            send_sem=side_send.at[slot],
            recv_sem=recv_sem.at[slot],
            device_id={"ep": chip * CORES + other},
        )

    def lanes_of(index):
        return pl.ds(pl.multiple_of(index * columns, columns), columns)

    def chip_copy(target):
        return pltpu.make_async_remote_copy(
            src_ref=normed_ref.at[:, lanes_of(tp_me)],
            dst_ref=tokens.at[me, :, lanes_of(tp_me)],
            send_sem=chip_send.at[target],
            recv_sem=piece_recv.at[me, tp_me],
            device_id={"ep": target * CORES + core},
        )

    def plane_copy(slot, piece, target):
        place = tokens.at[slot, :, lanes_of(piece)]
        return pltpu.make_async_remote_copy(
            src_ref=place,
            dst_ref=place,
            send_sem=plane_send.at[slot, target],
            recv_sem=piece_recv.at[slot, piece],
            device_id={"tp": target},
        )

    def block_copy(src, slot):
        return pltpu.make_async_remote_copy(
            src_ref=src,
            dst_ref=tokens.at[slot],
            send_sem=block_send.at[slot],
            recv_sem=block_recv.at[slot],
            device_id={"ep": chip * CORES + other},
        )

    loop(chips - 1, lambda turn: chip_copy(chip_at(turn)).start())

    @pl.when(chip < chips - 1)
    def _():
        up_copy(kv_ref, me).start()

    @pl.when(core == 0)
    def _():
        side_copy(kv_ref, me).start()

    block_copy(normed_ref, me).start()
    own_copy = pltpu.make_async_copy(normed_ref, tokens.at[me], own_sem)
    own_copy.start()
    loop(ep_count - 1, lambda turn: rank_copy(ep_at(turn), me).start())
    picks[me] = rank_ref[me]

    def spread_pieces(turn):
        slot = chip_at(turn) * CORES + core
        plane_copy(slot, tp_me, tp_me).wait_recv()
        loop(tp_count - 1, lambda way: plane_copy(slot, tp_me, tp_at(way)).start())

    def share_blocks(turn):
        slot = chip_at(turn) * CORES + core
        loop(tp_count - 1, lambda way: plane_copy(slot, tp_at(way), tp_me).wait_recv())
        block_copy(tokens.at[slot], slot).start()

    ones = jnp.ones((rows, LANES), jnp.bfloat16)

    def block_step(block, source, first):
        for pair in range(pairs):
            lanes = pl.ds(pair * LANES, LANES)
            value_lanes = pl.ds(width + pair * LANES, LANES)

            def one_tile(index, carry):
                start = pl.multiple_of(index * tile, tile)
                q_rows = pl.ds(start, tile)
                gates = gate_ref[pl.ds(pl.multiple_of(block * rows, rows), rows), lanes]
                keys = jnp.concatenate([source[:, lanes], gates], axis=1)
                values = jnp.concatenate([source[:, value_lanes], ones], axis=1)
                for head in range(2 * pair, min(2 * pair + 2, heads)):
                    scores = lax.dot_general(
                        q_ref[head, q_rows, :],
                        keys,
                        (((1,), (1,)), ((), ())),
                        preferred_element_type=jnp.float32,
                    )
                    if first:
                        q_pos = start + lax.broadcasted_iota(jnp.int32, scores.shape, 0)
                        k_pos = lax.broadcasted_iota(jnp.int32, scores.shape, 1)
                        scores = jnp.where(k_pos <= q_pos, scores, neg_fill)
                        top = jnp.max(scores, axis=1, keepdims=True)
                        new_max = jnp.broadcast_to(top, (tile, LANES))
                    else:
                        old_max = row_max[head, q_rows, :]
                        new_max = jnp.maximum(old_max, jnp.max(scores, axis=1, keepdims=True))
                    probs = jnp.exp(scores - new_max[:, :1]).astype(jnp.bfloat16)
                    add = jnp.dot(probs, values, preferred_element_type=jnp.float32)
                    if not first:
                        keep = jnp.exp(old_max - new_max)
                        add = add + acc[head, q_rows, :] * jnp.concatenate([keep, keep], axis=1)
                    acc[head, q_rows, :] = add
                    row_max[head, q_rows, :] = new_max
                return carry

            lax.fori_loop(0, tiles, one_tile, 0)

    block_step(me, kv_ref, True)
    loop(chips - 1, spread_pieces)

    @pl.when(me == 0)
    def _():
        loop(chips - 1, share_blocks)

    def remote_step(step, carry):
        turn = step - core + 2
        own_core = turn % 2 == 0
        slot = (chip - turn // 2) * CORES + jnp.where(own_core, core, other)
        landed = held.at[slot]
        side_copy(landed, slot).wait_recv()

        @pl.when(jnp.logical_and(own_core, chip < chips - 1))
        def _():
            up_copy(landed, slot).start()

        @pl.when(own_core)
        def _():
            side_copy(landed, slot).start()

        @pl.when(step == jnp.maximum(me - 2, 0))
        def _():
            loop(chips - 1, share_blocks)

        block_step(slot, landed, False)
        return carry

    lax.fori_loop(0, me, remote_step, 0)

    for head in range(heads):
        pair, part = head // 2, head % 2
        spot = slice(part * HEAD, part * HEAD + HEAD)
        whole = acc[head, :, :LANES] / acc[head, :, LANES:]
        out_ref[:, head * HEAD : (head + 1) * HEAD] = whole[:, spot].astype(out_ref.dtype)

    def finish(step):
        slot = (chip - step) * CORES + core

        @pl.when(chip < chips - 1)
        def _():
            up_copy(held.at[slot], slot).wait_send()

        @pl.when(step > 0)
        def _():
            side_copy(held.at[slot], slot).wait_send()

    loop(chip + 1, finish)

    @pl.when(core == 0)
    def _():
        side_copy(kv_ref, me).wait_send()

    def finish_tokens(turn):
        target = chip_at(turn)
        slot = target * CORES + core
        chip_copy(target).wait_send()
        loop(tp_count - 1, lambda way: plane_copy(slot, tp_me, tp_at(way)).wait_send())
        block_copy(tokens.at[slot], slot).wait_send()

    loop(chips - 1, finish_tokens)
    block_copy(normed_ref, me).wait_send()

    def finish_blocks(index):
        slot = index * CORES + other
        block_copy(tokens.at[slot], slot).wait_recv()

    loop(chips, finish_blocks)
    own_copy.wait()

    def finish_ranks(turn):
        rank_copy(ep_at(turn), me).wait_send()
        rank_copy(ep_at(turn), ep_at(turn)).wait_recv()

    loop(ep_count - 1, finish_ranks)


def exchange_kernel(count, *refs):
    sources, targets = refs[:count], refs[count : 2 * count]
    send_sem, recv_sem, own_sem = refs[2 * count :]
    tp_count = lax.axis_size("tp")
    tp_me = lax.axis_index("tp")
    barrier = pltpu.get_barrier_semaphore()
    ways = [lax.rem(tp_me + turn, tp_count) for turn in range(1, tp_count)]
    for way in ways:
        pl.semaphore_signal(barrier, inc=1, device_id={"tp": way})
    pl.semaphore_wait(barrier, tp_count - 1)

    def place(index, owner):
        span = sources[index].shape[1]
        if span % LANES:
            return targets[index].at[owner]
        return targets[index].at[:, pl.ds(pl.multiple_of(owner * span, span), span)]

    def copy(index, way, owner):
        return pltpu.make_async_remote_copy(
            src_ref=sources[index],
            dst_ref=place(index, owner),
            send_sem=send_sem.at[index, way],
            recv_sem=recv_sem.at[index, owner],
            device_id={"tp": way},
        )

    for index in range(count):
        for way in ways:
            copy(index, way, tp_me).start()
    own = [
        pltpu.make_async_copy(sources[index], place(index, tp_me), own_sem.at[index])
        for index in range(count)
    ]
    for one in own:
        one.start()
    for one in own:
        one.wait()
    for index in range(count):
        for way in ways:
            copy(index, way, way).wait_recv()
            copy(index, way, tp_me).wait_send()


def exchange(collective_id, *arrays):
    tp_count = lax.axis_size("tp")
    count = len(arrays)

    def gathered(a):
        rows, span = a.shape
        shape = (tp_count, rows, span) if span % LANES else (rows, tp_count * span)
        return jax.ShapeDtypeStruct(shape, a.dtype)

    results = pl.pallas_call(
        functools.partial(exchange_kernel, count),
        out_shape=[gathered(a) for a in arrays],
        in_specs=[pl.BlockSpec(memory_space=pltpu.VMEM)] * count,
        out_specs=[pl.BlockSpec(memory_space=pltpu.VMEM)] * count,
        scratch_shapes=[
            pltpu.SemaphoreType.DMA((count, tp_count)),
            pltpu.SemaphoreType.DMA((count, tp_count)),
            pltpu.SemaphoreType.DMA((count,)),
        ],
        compiler_params=pltpu.CompilerParams(collective_id=collective_id, has_side_effects=True),
        cost_estimate=pl.CostEstimate(flops=0, bytes_accessed=24 * 1024 * 1024, transcendentals=0),
        name="exchange",
    )(*arrays)
    return [
        r if r.ndim == 2 else r.transpose(1, 0, 2).reshape(r.shape[1], -1) for r in results
    ]


def attention(query_rows, key_rows, value_rows, cum_gate, normed, ranks):
    rows, width = query_rows.shape
    heads = width // HEAD
    pairs = (heads + 1) // 2
    ep_count = lax.axis_size("ep")
    padded = pairs * LANES
    if padded > width:
        spare = ((0, 0), (0, padded - width))
        query_rows, key_rows, value_rows = (
            jnp.pad(a, spare) for a in (query_rows, key_rows, value_rows)
        )
    key_value = jnp.concatenate([key_rows, value_rows], axis=1)
    scaled = query_rows * jnp.asarray(HEAD**-0.5, jnp.bfloat16)
    lane = jnp.arange(LANES)
    parts = []
    for head in range(heads):
        pair, part = head // 2, head % 2
        piece = scaled[:, pair * LANES : (pair + 1) * LANES]
        piece = jnp.where((lane // HEAD == part)[None], piece, 0)
        marks = ((lane // 3) == part).astype(jnp.bfloat16)
        parts.append(jnp.concatenate([piece, jnp.broadcast_to(marks, (rows, LANES))], axis=1))
    queries = jnp.stack(parts)
    minus = -cum_gate
    high = lax.reduce_precision(minus, 8, 7)
    rest = minus - high
    mid = lax.reduce_precision(rest, 8, 7)
    low = rest - mid
    terms = jnp.concatenate([high, mid, low], axis=0).astype(jnp.bfloat16)
    source = jnp.arange(3 * heads)
    spot = (source % heads // 2) * LANES + (source % heads % 2) * 3 + source // heads
    layout = (spot[:, None] == jnp.arange(padded)[None, :]).astype(jnp.bfloat16)
    gates = lax.dot_general(
        terms, layout, (((0,), (0,)), ((), ())), preferred_element_type=jnp.float32
    ).astype(jnp.bfloat16)
    blocks = ep_count * rows * rows * heads
    return pl.pallas_call(
        functools.partial(attention_kernel, heads),
        out_shape=[
            jax.ShapeDtypeStruct((rows, heads * HEAD), jnp.bfloat16),
            jax.ShapeDtypeStruct((ep_count,) + normed.shape, jnp.bfloat16),
            jax.ShapeDtypeStruct(ranks.shape, jnp.bfloat16),
        ],
        in_specs=[pl.BlockSpec(memory_space=pltpu.VMEM)] * 5,
        out_specs=[
            pl.BlockSpec(memory_space=pltpu.VMEM),
            pl.BlockSpec(memory_space=pl.ANY),
            pl.BlockSpec(memory_space=pltpu.VMEM),
        ],
        scratch_shapes=[
            pltpu.VMEM((ep_count, rows, 2 * padded), jnp.bfloat16),
            pltpu.VMEM((heads, rows, 2 * LANES), jnp.float32),
            pltpu.VMEM((heads, rows, LANES), jnp.float32),
            pltpu.SemaphoreType.DMA((ep_count,)),
            pltpu.SemaphoreType.DMA((ep_count,)),
            pltpu.SemaphoreType.DMA((ep_count,)),
            pltpu.SemaphoreType.DMA((ep_count,)),
            pltpu.SemaphoreType.DMA((ep_count, lax.axis_size("tp"))),
            pltpu.SemaphoreType.DMA((ep_count, lax.axis_size("tp"))),
            pltpu.SemaphoreType.DMA((ep_count,)),
            pltpu.SemaphoreType.DMA((ep_count,)),
            pltpu.SemaphoreType.DMA,
            pltpu.SemaphoreType.DMA((ep_count,)),
            pltpu.SemaphoreType.DMA((ep_count,)),
        ],
        compiler_params=pltpu.CompilerParams(
            collective_id=0, has_side_effects=True, vmem_limit_bytes=48 * 1024 * 1024
        ),
        cost_estimate=pl.CostEstimate(
            flops=blocks * 2 * 512, bytes_accessed=8 * 1024 * 1024, transcendentals=blocks
        ),
        name="attend",
    )(queries, key_value, gates, normed, ranks)


def local(
    query_rows,
    key_rows,
    value_rows,
    cum_gate,
    out_weight,
    moe_input,
    moe_gain,
    routes,
    route_weight,
    expert_gate,
    expert_up,
    expert_down,
    shared_gate,
    shared_up,
    shared_down,
):
    token_count = moe_input.shape[0]
    top_count = routes.shape[1]
    local_experts = expert_gate.shape[0]
    ep_count = lax.axis_size("ep")
    expert_count = local_experts * ep_count
    capacity = 2 * token_count * top_count // expert_count
    column_count = expert_down.shape[2]
    first_column = lax.axis_index("tp") * column_count
    moe_rows = moe_input.astype(jnp.float32)
    normed = (
        moe_rows
        * lax.rsqrt(jnp.mean(moe_rows * moe_rows, axis=1, keepdims=True) + norm_eps)
        * moe_gain
    ).astype(jnp.bfloat16)
    expert_ids = jnp.arange(expert_count, dtype=jnp.int32)
    chosen = routes[:, :, None] == expert_ids[None, None, :]
    named = jnp.any(chosen, axis=1)
    weight_of = jnp.sum(jnp.where(chosen, route_weight[:, :, None], 0.0), axis=1)
    order = jnp.arange(token_count)
    earlier = (order[None, :] < order[:, None]).astype(jnp.bfloat16)
    ranks = jnp.dot(earlier, named.astype(jnp.bfloat16), preferred_element_type=jnp.float32)
    ranks = jnp.where(named, ranks.astype(jnp.int32), -1)
    slots = jnp.arange(capacity, dtype=jnp.int32)
    place = ranks[:, :, None] == slots[None, None, :]
    rank_rows = ranks.astype(jnp.bfloat16).T.reshape(ep_count, local_experts, token_count)
    heads_out, tokens, mine = attention(
        query_rows, key_rows, value_rows, cum_gate, normed, rank_rows
    )
    pick = mine[:, :, None, :] == slots.astype(jnp.bfloat16)[None, None, :, None]
    pick = pick.astype(jnp.bfloat16).reshape(ep_count, local_experts * capacity, token_count)
    arrived = jnp.einsum("ast,atd->asd", pick, tokens, preferred_element_type=jnp.float32)
    arrived = arrived.astype(jnp.bfloat16).reshape(ep_count, local_experts, capacity, -1)
    gate_val = jnp.einsum(
        "aecd,edf->aecf", arrived, expert_gate, preferred_element_type=jnp.float32
    )
    up_val = jnp.einsum("aecd,edf->aecf", arrived, expert_up, preferred_element_type=jnp.float32)
    hidden = (jax.nn.silu(gate_val) * up_val).astype(jnp.bfloat16)
    shared_hidden = (
        jax.nn.silu(jnp.dot(normed, shared_gate, preferred_element_type=jnp.float32))
        * jnp.dot(normed, shared_up, preferred_element_type=jnp.float32)
    ).astype(jnp.bfloat16)
    slot_count = ep_count * local_experts * capacity
    by_expert = hidden.transpose(1, 0, 2, 3).reshape(slot_count, hidden.shape[3])
    hidden, shared_all = exchange(1, by_expert, shared_hidden)
    hidden = hidden.reshape(local_experts, ep_count * capacity, -1)
    result = jnp.einsum("esf,efd->esd", hidden, expert_down, preferred_element_type=jnp.float32)
    result = result.astype(jnp.bfloat16).reshape(local_experts, ep_count, capacity, column_count)
    result = result.transpose(1, 0, 2, 3)
    result, heads_out = lax.optimization_barrier((result, heads_out))
    returned = lax.all_to_all(result, "ep", split_axis=0, concat_axis=0, tiled=True)
    returned = returned.reshape(expert_count * capacity, column_count)
    weight_high = lax.reduce_precision(weight_of, 8, 7)
    weight_low = weight_of - weight_high
    routed = 0.0
    for weight in (weight_high, weight_low):
        spread = jnp.where(place, weight[:, :, None], 0.0).astype(jnp.bfloat16)
        routed = routed + jnp.dot(
            spread.reshape(token_count, expert_count * capacity),
            returned,
            preferred_element_type=jnp.float32,
        )
    (heads_all,) = exchange(2, heads_out)
    mixer_sum = jnp.dot(heads_all, out_weight, preferred_element_type=jnp.float32)
    moe_total = routed + jnp.dot(shared_all, shared_down, preferred_element_type=jnp.float32)
    return (mixer_sum.astype(jnp.bfloat16), moe_total.astype(jnp.bfloat16))


def solution(mesh):
    placed = (
        P("ep", "tp"),
        P("ep", "tp"),
        P("ep", "tp"),
        P("tp", None),
        P(None, "tp"),
        P("ep", None),
        P(),
        P("ep", None),
        P("ep", None),
        P("ep", None, "tp"),
        P("ep", None, "tp"),
        P("ep", None, "tp"),
        P(None, "tp"),
        P(None, "tp"),
        P(None, "tp"),
    )
    return jax.shard_map(
        local, mesh=mesh, in_specs=placed, out_specs=(P("ep", "tp"), P("ep", "tp")), check_vma=False
    )
```
